512 devices in a mesh: sp: 64 (over z, y), tp: 8 (over x, core).
Axes of the slice: x: 4, y: 8, z: 8, core: 2. Of those that a mesh axis runs over, the one named last changes fastest.
Arguments:
- features: bfloat16 [16384, 2048], P('sp'), may hold values from -16 to 16
- value_weight: bfloat16 [2048, 1024], P(None, 'tp'), may hold values from -0.125 to 0.125
- queries: bfloat16 [16384, 512], P('sp', 'tp'), may hold values from -9 to 9
- key_vectors: bfloat16 [16384, 512], P('sp', 'tp'), may hold values from -0.17 to 0.17
- log_input: float32 [2, 8, 16384], P(None, 'tp', 'sp'), may hold values from -6 to 100
- log_forget: float32 [2, 8, 16384], P(None, 'tp', 'sp'), may hold values from -3 to 0, as said below
- out_grad: bfloat16 [16384, 1024], P('sp', 'tp'), may hold values from -6 to 6
Outputs:
- grad_queries: bfloat16 [16384, 512], P('sp', 'tp')
- grad_keys: bfloat16 [16384, 512], P('sp', 'tp')
- grad_log_input: float32 [2, 8, 16384], P(None, 'tp', 'sp')
- grad_log_forget: float32 [2, 8, 16384], P(None, 'tp', 'sp')
- grad_weight: float32 [2048, 1024], P('sp', 'tp')
- grad_features: bfloat16 [16384, 2048], P(('sp', 'tp'))
The draws below stay inside these ranges and needn't reach their ends.
Inputs may be any that keep to these rules, and one draw needn't show every extreme that they name: `log_forget`: every entry is below zero.
All inputs are finite; a program needn't handle non-finite values.
Results may differ from the reference program's by a relative error of at most 0.013.
Values may be sent and summed in bfloat16 or wider, within the bound.
A program may use at most 64 MiB of HBM per device.

```python
import jax
import jax.numpy as jnp
from jax import lax

D = 2048
HEADS = 8
DK = 64
DV = 128
TOK_DEV = 256
TOKENS = 16384
N_SP = 64
N_TP = 8


def shared_direction(key):
    signs = jax.random.randint(jax.random.fold_in(key, 5), (HEADS, DK), 0, 2).astype(jnp.float32)
    return jnp.tile((2.0 * signs - 1.0).reshape(1, HEADS * DK), (TOKENS, 1))


def draw_queries(key, part):
    noise = jnp.clip(jax.random.normal(jax.random.fold_in(key, 41), (TOKENS, HEADS * DK), jnp.float32), -6.0, 6.0)
    return (noise + 2.5 * shared_direction(key)).astype(jnp.bfloat16)


def draw_key_vectors(key, part):
    noise = jnp.clip(jax.random.normal(jax.random.fold_in(key, 43), (TOKENS, HEADS * DK), jnp.float32), -6.0, 6.0)
    return (0.02 * (noise + 2.5 * shared_direction(key))).astype(jnp.bfloat16)


def draw_log_input(key, part):
    streams = jax.random.split(jax.random.fold_in(key, 17), 1)
    noise = jax.random.normal(streams[0], (2, HEADS, TOKENS), jnp.float32)
    return jnp.clip(1.5 * noise - 1.0, -6.0, 3.0)


def draw_log_forget(key, part):
    streams = jax.random.split(jax.random.fold_in(key, 29), 6)
    slow = jax.random.uniform(streams[0], (2, HEADS, 1), jnp.float32) < 0.5
    noise = jnp.clip(0.5 * jax.random.normal(streams[1], (2, HEADS, TOKENS), jnp.float32), -1.5, 1.5)
    fast_rate = 1.0 / min(40, max(TOK_DEV // 2, 2))
    slow_rate = 0.5 / TOKENS
    base = jnp.where(slow, slow_rate, fast_rate)
    steps_log = jax.random.randint(streams[2], (2, HEADS, TOKENS // TOK_DEV), -1, 2).astype(jnp.float32)
    jitter = jax.random.uniform(streams[3], (2, HEADS, TOKENS // TOK_DEV), jnp.float32, -0.3, 0.3)
    factor = jnp.repeat(jnp.exp2(steps_log) * jnp.exp(jitter), TOK_DEV, axis=2)
    rate = base * jnp.exp(noise) * factor
    spots = jax.random.randint(streams[4], (2, HEADS, 4), 0, TOKENS)
    places = jnp.arange(TOKENS, dtype=jnp.int32)
    marked = jnp.any(places[None, None, :, None] == spots[:, :, None, :], axis=-1)
    depth = jax.random.uniform(streams[5], (2, HEADS, TOKENS), jnp.float32, 0.22, 0.69)
    return jnp.clip(jnp.where(marked, -depth, -rate), -3.0, -1e-07)


def strengthened(values, stream_key, source, target, shards_of, factor):
    owner, partner = [(jnp.arange(values.shape[dim]) // (values.shape[dim] // shards_of)).reshape([-1 if axis == dim else 1 for axis in range(values.ndim)]) for dim in (source, target)]
    chosen = jax.random.permutation(stream_key, shards_of)[partner]
    strong = (owner == chosen) | (owner == (partner + shards_of // 2) % shards_of)
    return jnp.where(strong, factor * values, values)


def block_levels(own_key, shape, shards, low, high):
    factor_of = 1.0
    for axis_at, blocks in shards:
        draws = jax.random.uniform(jax.random.fold_in(jax.random.fold_in(own_key, 6), axis_at), (blocks,), jnp.float32, low / len(shards), high / len(shards))
        factor_of = factor_of * jnp.repeat(jnp.exp(draws), shape[axis_at] // blocks).reshape((-1,) + (1,) * (len(shape) - 1 - axis_at))
    return factor_of


def gaussian(own_key, shape, scale, reach, pieces=(), kind=jnp.bfloat16):
    entries = jax.random.normal(own_key, shape, jnp.float32) * scale
    if len(pieces) > 0:
        entries = block_levels(own_key, shape, pieces, -0.22, 0.18) * entries
    return jnp.clip(entries, min=-reach, max=reach).astype(kind)


def noise_with(rng, extent, deviation, most, shards, heavy, held_as=jnp.bfloat16):
    values = deviation * jax.random.normal(rng, extent, jnp.float32)
    if shards:
        values = values * block_levels(rng, extent, shards, -0.22, 0.18)
    return jnp.clip(strengthened(values, jax.random.fold_in(rng, 3), *heavy), -most, most).astype(held_as)


def setup_inputs(seed: int = 0) -> dict:
    keys = jax.random.split(jax.random.key(seed), 8)
    return {
        "features": noise_with(keys[0], (TOKENS, D), 1.0, 16.0, ((0, 64),), (0, 1, 64, 4.0)),
        "value_weight": gaussian(keys[1], (D, HEADS * DV), D ** -0.5, 0.125, ((1, 8),)),
        "queries": draw_queries(jax.random.fold_in(keys[7], 71), 0),
        "key_vectors": draw_key_vectors(jax.random.fold_in(keys[7], 71), 0),
        "log_input": draw_log_input(jax.random.fold_in(keys[7], 71), 0),
        "log_forget": draw_log_forget(jax.random.fold_in(keys[7], 71), 0),
        "out_grad": gaussian(keys[6], (TOKENS, HEADS * DV), 1.0, 6.0, ((0, 64), (1, 8))),
    }


peak_exponent = lax.Precision.HIGHEST
very_low = -1.0e30


def summarize(float_keys, float_values, log_in, log_fg):
    cumulative = jnp.cumsum(log_fg, axis=1)
    decay_sum = cumulative[:, -1]
    exponent = decay_sum[:, None] - cumulative + log_in
    top_log = jnp.max(exponent, axis=1)
    weight = jnp.exp(exponent - top_log[:, None])
    weighted_terms = float_keys * weight[:, :, None]
    memory_matrix = jnp.einsum('cxr,cxy->cry', weighted_terms, float_values, precision=peak_exponent)
    normalizer = jnp.sum(weighted_terms, axis=1)
    return cumulative, (decay_sum, memory_matrix, normalizer, top_log)


def combine(earlier, latter):
    decay_sum = earlier[0] + latter[0]
    top_log = jnp.maximum(earlier[3] + latter[0], latter[3])
    factor_one = jnp.exp(earlier[3] + latter[0] - top_log)
    factor_two = jnp.exp(latter[3] - top_log)
    memory_matrix = factor_one[..., None, None] * earlier[1] + factor_two[..., None, None] * latter[1]
    normalizer = factor_one[..., None] * earlier[2] + factor_two[..., None] * latter[2]
    return (decay_sum, memory_matrix, normalizer, top_log)


def empty_state(head_count, rows_count, width):
    return (jnp.zeros((head_count,), jnp.float32), jnp.zeros((head_count, rows_count, width), jnp.float32),
            jnp.zeros((head_count, rows_count), jnp.float32), jnp.full((head_count,), very_low, jnp.float32))


def forward_part(query_b, keys_b, values_b, grad_b, log_in, cumulative, incoming):
    incoming_memory, normalizer_in, top_in = incoming
    float_query = query_b.astype(jnp.float32)
    float_keys = keys_b.astype(jnp.float32)
    float_values = values_b.astype(jnp.float32)
    grad_f = grad_b.astype(jnp.float32)
    length = cumulative.shape[1]
    places = lax.iota(jnp.int32, length)
    causal_mask = (places[:, None] >= places[None, :])[None]
    exponent = jnp.where(causal_mask, cumulative[:, :, None] - cumulative[:, None, :] + log_in[:, None, :], very_low)
    carry_log = cumulative + top_in[:, None]
    top_log = jnp.maximum(carry_log, jnp.max(exponent, axis=2))
    weight = jnp.where(causal_mask, jnp.exp(exponent - top_log[:, :, None]), 0.0)
    carried_over = jnp.exp(carry_log - top_log)
    scores = jnp.einsum('htk,hsk->hts', float_query, float_keys, precision=peak_exponent)
    scored = weight * scores
    numerator_term = (carried_over[..., None] * jnp.einsum('gsd,gdi->gsi', float_query, incoming_memory, precision=peak_exponent)
                 + jnp.einsum('hts,hsv->htv', scored, float_values, precision=peak_exponent))
    denominator = carried_over * jnp.sum(float_query * normalizer_in[:, None, :], axis=2) + jnp.sum(scored, axis=2)
    floor_value = jnp.exp(-top_log)
    divisor = jnp.maximum(jnp.abs(denominator), floor_value)
    hidden = numerator_term / divisor[..., None]
    numerator_gradient = grad_f / divisor[..., None]
    grad_denom = jnp.where(jnp.abs(denominator) > floor_value,
                           -jnp.sign(denominator) * jnp.sum(grad_f * hidden, axis=2) / divisor, 0.0)
    raw_pairing = jnp.einsum('htv,hsv->hts', grad_f, float_values, precision=peak_exponent)
    pairing = raw_pairing / divisor[..., None] + grad_denom[..., None]
    masked = weight * pairing
    grad_query = (jnp.einsum('hts,hsk->htk', masked, float_keys, precision=peak_exponent)
                  + carried_over[..., None] * (jnp.einsum('pfr,pdr->pdf', incoming_memory, numerator_gradient, precision=peak_exponent)
                                          + normalizer_in[:, None, :] * grad_denom[..., None]))
    key_local = jnp.einsum('hts,htk->hsk', masked, float_query, precision=peak_exponent)
    value_local = jnp.einsum('hts,htv->hsv', scored, numerator_gradient, precision=peak_exponent)
    row_total = jnp.sum(numerator_gradient * numerator_term, axis=2) + grad_denom * denominator
    back_log = cumulative - top_log
    back_top = jnp.max(back_log, axis=1)
    reverse_weight_factor = jnp.exp(back_log - back_top[:, None])
    memory_gradient = jnp.einsum('cxr,cxy->cry', float_query * reverse_weight_factor[..., None], numerator_gradient, precision=peak_exponent)
    normalizer_gradient = jnp.sum(float_query * (reverse_weight_factor * grad_denom)[..., None], axis=1)
    return grad_query, key_local, value_local, row_total, (memory_gradient, normalizer_gradient, back_top)


def backward_part(float_keys, float_values, log_in, cumulative, decay_sum, key_local, value_local, row_total,
                  incoming_state, incoming_grad):
    incoming_memory, normalizer_in, top_in = incoming_state
    memory_gradient, normalizer_gradient, grad_top = incoming_grad
    scaling = jnp.exp(log_in + decay_sum[:, None] - cumulative + grad_top[:, None])
    passed_key_sum = jnp.einsum('xqy,xty->xtq', memory_gradient, float_values, precision=peak_exponent) + normalizer_gradient[:, None, :]
    passed_value_sum = jnp.einsum('nfp,nxf->nxp', memory_gradient, float_keys, precision=peak_exponent)
    grad_key = key_local + scaling[..., None] * passed_key_sum
    grad_value = value_local + scaling[..., None] * passed_value_sum
    local_column = jnp.sum(float_keys * key_local, axis=2)
    carried_column = scaling * jnp.sum(float_keys * passed_key_sum, axis=2)
    grad_in = local_column + carried_column
    across = jnp.exp(top_in + decay_sum + grad_top) * (jnp.sum(incoming_memory * memory_gradient, axis=(1, 2))
                                                       + jnp.sum(normalizer_in * normalizer_gradient, axis=1))
    suffix = jnp.flip(jnp.cumsum(jnp.flip(row_total - local_column, 1), axis=1), 1)
    prefix = jnp.cumsum(carried_column, axis=1) - carried_column
    grad_fg = suffix + prefix + across[:, None]
    return grad_key, grad_value, grad_in, grad_fg


def to_blocks(tensor):
    shaped = tensor.reshape(tensor.shape[:1] + (N_SP, TOK_DEV) + tensor.shape[2:])
    return jnp.moveaxis(shaped, 1, 0)


def from_blocks(tensor):
    moved = jnp.moveaxis(tensor, 0, 1)
    return moved.reshape(moved.shape[:1] + (TOKENS,) + moved.shape[3:])


def one_direction(query_h, keys_h, values_h, grad_h, log_in, log_fg):
    head_count = query_h.shape[0]
    query_b, keys_b, values_b, grad_b = to_blocks(query_h), to_blocks(keys_h), to_blocks(values_h), to_blocks(grad_h)
    keys_fb = keys_b.astype(jnp.float32)
    values_fb = values_b.astype(jnp.float32)
    in_b, fg_b = to_blocks(log_in), to_blocks(log_fg)
    cumul_b, summaries = jax.vmap(summarize)(keys_fb, values_fb, in_b, fg_b)

    def advance(running, element):
        return combine(running, element), running

    start_state = empty_state(head_count, keys_h.shape[2], values_h.shape[2])
    unused, states_in = lax.scan(advance, start_state, summaries)

    def run_forward(packed):
        return forward_part(packed[0], packed[1], packed[2], packed[3], packed[4], packed[5],
                            (packed[6], packed[7], packed[8]))

    grad_q, key_loc, value_loc, rows_b, grad_sum = lax.map(
        run_forward, (query_b, keys_b, values_b, grad_b, in_b, cumul_b, states_in[1], states_in[2], states_in[3]))
    elements = (summaries[0], grad_sum[0], grad_sum[1], grad_sum[2])
    unused, grads_in = lax.scan(advance, start_state, elements, reverse=True)

    def run_backward(packed):
        return backward_part(packed[0], packed[1], packed[2], packed[3], packed[4], packed[5], packed[6],
                             packed[7], (packed[8], packed[9], packed[10]), (packed[11], packed[12], packed[13]))

    grad_k, grad_v, grad_i, grad_f_out = lax.map(
        run_backward, (keys_fb, values_fb, in_b, cumul_b, summaries[0], key_loc, value_loc, rows_b,
                       states_in[1], states_in[2], states_in[3], grads_in[1], grads_in[2], grads_in[3]))
    return (from_blocks(grad_q), from_blocks(grad_k), from_blocks(grad_v),
            from_blocks(grad_i), from_blocks(grad_f_out))


def to_heads(tensor, width):
    return tensor.reshape(TOKENS, HEADS, width).transpose(1, 0, 2)


def reference(features, value_weight, queries, key_vectors, log_input, log_forget, out_grad):
    values = jnp.dot(features, value_weight, preferred_element_type=jnp.float32).astype(jnp.bfloat16)
    query_h = to_heads(queries, DK)
    key_h = to_heads(key_vectors, DK)
    value_h = to_heads(values, DV)
    grad_h = to_heads(out_grad, DV)
    outputs = []
    for direction in range(2):
        if direction == 1:
            packed = [jnp.flip(tensor, 1) for tensor in (query_h, key_h, value_h, grad_h,
                                                         log_input[direction], log_forget[direction])]
        else:
            packed = [query_h, key_h, value_h, grad_h, log_input[direction], log_forget[direction]]
        result = one_direction(packed[0], packed[1], packed[2], packed[3], packed[4], packed[5])
        if direction == 1:
            result = tuple(jnp.flip(tensor, 1) for tensor in result)
        outputs.append(result)
    grad_q = outputs[0][0] + outputs[1][0]
    grad_k = outputs[0][1] + outputs[1][1]
    grad_v = outputs[0][2] + outputs[1][2]
    grad_queries = grad_q.transpose(1, 0, 2).reshape(TOKENS, HEADS * DK).astype(jnp.bfloat16)
    grad_keys = grad_k.transpose(1, 0, 2).reshape(TOKENS, HEADS * DK).astype(jnp.bfloat16)
    grad_values = grad_v.transpose(1, 0, 2).reshape(TOKENS, HEADS * DV).astype(jnp.bfloat16)
    grad_log_input = jnp.stack([outputs[0][3], outputs[1][3]])
    grad_log_forget = jnp.stack([outputs[0][4], outputs[1][4]])
    grad_weight = jnp.dot(features.T, grad_values, preferred_element_type=jnp.float32)
    group_width = (HEADS // N_TP) * DV
    summed = jnp.zeros((TOKENS, D), jnp.float32)
    for member in range(N_TP):
        columns = grad_values[:, member * group_width:(member + 1) * group_width]
        weights_part = value_weight[:, member * group_width:(member + 1) * group_width]
        partial_sum = jnp.dot(columns, weights_part.T, preferred_element_type=jnp.float32)
        summed = summed + lax.optimization_barrier(partial_sum.astype(jnp.bfloat16)).astype(jnp.float32)
    grad_features = summed.astype(jnp.bfloat16)
    return (grad_queries, grad_keys, grad_log_input, grad_log_forget, grad_weight, grad_features)
```

```python
import jax
import jax.numpy as jnp
from jax import lax
from jax.experimental import pallas as pl
from jax.experimental.pallas import tpu as pltpu
from jax.sharding import PartitionSpec as P

DK = 64
DV = 128
TOK = 256
D = 2048
SIDE = 8
N_TP = 8
ROWS = D // 64

LOW = -1e30
F32 = jnp.float32
BF16 = jnp.bfloat16
MESH = pl.DeviceIdType.MESH

(N1, N2, M1, M2, M3, G1, G2, G3, H1, H2, A1, B1, A2, B2, VX, VC, GV, KINDS) = range(18)


def dot(a, b, da, db):
    return lax.dot_general(a, b, (((da,), (db,)), ((), ())), preferred_element_type=F32)


def halves(x):
    high = x.astype(BF16)
    return high, (x - high.astype(F32)).astype(BF16)


def dot_left(x, b, da, db):
    high, low = halves(x)
    return dot(high, b, da, db) + dot(low, b, da, db)


def dot_right(a, x, da, db):
    high, low = halves(x)
    return dot(a, high, da, db) + dot(a, low, da, db)


def kernel(
    f_ref, vw_ref, q_ref, k_ref, li_ref, lf_ref, g_ref,
    gq_out, gk_out, gi_out, gf_out, gw_out, gx_out,
    v_s, ft, w_s, s_s, r_s, p_s, u_s,
    n_send, n_buf, nz_send, nz_buf,
    m_send, m_buf, mz_send, mz_buf, mr_send, mr_buf,
    g_send, g_buf, gz_send, gz_buf, gr_send, gr_buf,
    h_send, h_buf, hz_send, hz_buf,
    wa_send, wa_buf, wb_send, wb_buf, wa2_send, wa2_buf, wb2_send, wb2_buf,
    vall, gv_s, gv_buf, ssem, rsem, lsem,
):
    sp = lax.axis_index("sp")
    tp = lax.axis_index("tp")
    z, y = lax.div(sp, SIDE), lax.rem(sp, SIDE)
    x, core = lax.div(tp, 2), lax.rem(tp, 2)

    def peer_id(axis, p):
        if axis == "y":
            return {"sp": z * SIDE + p}
        if axis == "z":
            return {"sp": p * SIDE + y}
        return {"tp": p}

    own = {"y": y, "z": z, "tp": tp}

    def copy(kind, axis, p, src, dst, slot):
        return pltpu.make_async_remote_copy(
            src_ref=src, dst_ref=dst, send_sem=ssem.at[kind, p], recv_sem=rsem.at[kind, slot],
            device_id=peer_id(axis, p), device_id_type=MESH,
        )

    def send_all(kind, axis, src_of, buf):
        me = own[axis]

        def step(i, c):
            p = lax.rem(me + i, SIDE)
            copy(kind, axis, p, src_of(p), buf.at[me], me).start()
            return c

        lax.fori_loop(1, SIDE, step, 0)

    def recv_all(kind, axis, buf):
        me = own[axis]

        def step(i, c):
            p = lax.rem(me + i, SIDE)
            copy(kind, axis, p, buf.at[p], buf.at[p], p).wait_recv()
            return c

        lax.fori_loop(1, SIDE, step, 0)

    def sent_all(kind, axis, src_of, buf):
        me = own[axis]

        def step(i, c):
            p = lax.rem(me + i, SIDE)
            copy(kind, axis, p, src_of(p), buf.at[me], me).wait_send()
            return c

        lax.fori_loop(1, SIDE, step, 0)

    barrier = pltpu.get_barrier_semaphore()
    for axis in ("y", "z", "tp"):
        def greet(i, c, axis=axis):
            p = lax.rem(own[axis] + i, SIDE)
            pl.semaphore_signal(barrier, inc=1, device_id=peer_id(axis, p), device_id_type=MESH)
            return c

        lax.fori_loop(1, SIDE, greet, 0)

    place = pltpu.make_async_copy(vw_ref, vall.at[tp], lsem)
    place.start()

    values = jnp.dot(f_ref[...], vw_ref[...], preferred_element_type=F32).astype(BF16)
    v_s[...] = values
    at_t = lax.broadcasted_iota(jnp.int32, (TOK, TOK), 0)
    at_s = lax.broadcasted_iota(jnp.int32, (TOK, TOK), 1)
    same = at_t == at_s
    reach = (at_s <= at_t, at_s >= at_t)
    lane = lax.broadcasted_iota(jnp.int32, (1, 2 * DK), 1)
    first = lane < DK
    sub = lax.broadcasted_iota(jnp.int32, (8, 2 * DK), 0)

    def column(row):
        return jnp.sum(jnp.where(same, row, 0.0), axis=1, keepdims=True)

    def row_of(col):
        return jnp.sum(jnp.where(same, col, 0.0), axis=0, keepdims=True)

    def pack(a, b):
        return jnp.where(first, a, b)

    def half_sum(packed):
        return (
            jnp.sum(jnp.where(first, packed, 0.0), axis=1, keepdims=True),
            jnp.sum(jnp.where(first, 0.0, packed), axis=1, keepdims=True),
        )

    c_col, i_row, c_row, end, ending, decay, top = [], [], [], [], [], [], []
    for d in range(2):
        l_row = lf_ref[d]
        in_row = li_ref[d]
        c = jnp.sum(jnp.where(reach[d], l_row, 0.0), axis=1, keepdims=True)
        cr = row_of(c)
        total = c[TOK - 1 :, :] if d == 0 else c[:1, :]
        e = total - c + column(in_row)
        peak = jnp.max(e, axis=0, keepdims=True)
        c_col.append(c)
        c_row.append(cr)
        i_row.append(in_row)
        ending.append(e)
        decay.append(total)
        top.append(peak)
    key2 = jnp.concatenate([k_ref[...], k_ref[...]], axis=1).astype(F32)
    weighted = key2 * pack(jnp.exp(ending[0] - top[0]), jnp.exp(ending[1] - top[1]))
    norm = jnp.sum(weighted, axis=0, keepdims=True)
    decay2 = pack(decay[0], decay[1])
    top2 = pack(top[0], top[1])

    def tile(a, b, c):
        return jnp.where(sub == 0, a, jnp.where(sub == 1, b, jnp.where(sub == 2, c, 0.0)))

    n_send[...] = tile(norm, decay2, top2)
    n_buf[y] = n_send[...]
    pl.semaphore_wait(barrier, 3 * (SIDE - 1))
    send_all(N1, "y", lambda p: n_send, n_buf)

    memory = dot_left(weighted, values, 0, 0)
    m_send[:, 0] = memory[:DK].reshape(SIDE, 8, DV)
    m_send[:, 1] = memory[DK:].reshape(SIDE, 8, DV)
    m_buf[y] = m_send[y]
    send_all(M1, "y", lambda p: m_send.at[p], m_buf)

    mate = x * 2 + (1 - core)
    for i in range(1, 4):
        p = lax.rem(x + i, 4) * 2 + core
        copy(VX, "tp", p, vw_ref, vall.at[tp], tp).start()
    copy(VC, "tp", mate, vw_ref, vall.at[tp], tp).start()

    scores = dot(q_ref[...], k_ref[...], 1, 1)
    s_s[...] = scores
    r_s[...] = dot(g_ref[...], v_s[...], 1, 1)
    m_local, den_local, num_local = [], [], []
    for d in range(2):
        e = jnp.where(reach[d], c_col[d] - c_row[d] + i_row[d], LOW)
        peak = jnp.max(e, axis=1, keepdims=True)
        w = jnp.exp(e - peak)
        w_s[d] = w
        ws = w * s_s[...]
        m_local.append(peak)
        den_local.append(jnp.sum(ws, axis=1, keepdims=True))
        num_local.append(jnp.sum(ws * r_s[...], axis=1, keepdims=True))

    def element(tiles, i, flip, rows):
        near, far = tiles[i], tiles[SIDE - 1 - i]
        take = first if not flip else jnp.logical_not(first)
        return [jnp.where(take, near[r : r + 1], far[r : r + 1]) for r in rows]

    def included(i, at, flip):
        low = jnp.where(i < at, 1, 0)
        high = jnp.where(SIDE - 1 - i > at, 1, 0)
        if flip:
            low, high = high, low
        return jnp.where(first, low, high) > 0

    empty = jnp.full((1, 2 * DK), LOW, F32)

    def chain(decays, tops, start, masks):
        run, past, factors = start, jnp.zeros((1, 2 * DK), F32), []
        for i in range(SIDE):
            dec, high = decays[i], tops[i]
            if masks is not None:
                dec = jnp.where(masks[i], dec, 0.0)
                high = jnp.where(masks[i], high, LOW)
            new = jnp.maximum(run + dec, high)
            keep = jnp.exp(run + dec - new)
            add = jnp.exp(high - new)
            if masks is not None:
                add = jnp.where(masks[i], add, 0.0)
            factors.append((keep, add))
            run, past = new, past + dec
        return run, past, factors

    def fold_rows(rows, factors):
        acc = jnp.zeros((1, 2 * DK), F32)
        for row, (keep, add) in zip(rows, factors):
            acc = keep * acc + add * row
        return acc

    def both(factor):
        return factor[:, :1], factor[:, DK : DK + 1]

    def fold_tiles(buf, factors, flip, start, store):
        acc = list(start)
        for i in range(SIDE):
            keep, add = both(factors[i][0]), both(factors[i][1])
            places = (i, SIDE - 1 - i) if not flip else (SIDE - 1 - i, i)
            for d in range(2):
                if store is not None:
                    store[places[d], d] = acc[d]
                acc[d] = keep[d] * acc[d] + add[d] * buf[places[d], d]
        return acc

    zero_tile = jnp.zeros((8, DV), F32)

    recv_all(N1, "y", n_buf)
    tiles_y = [n_buf[i] for i in range(SIDE)]
    els = [element(tiles_y, i, False, (0, 1, 2)) for i in range(SIDE)]
    norms_y, decays_y, tops_y = zip(*els)
    row_top, row_decay, total_f = chain(decays_y, tops_y, empty, None)
    row_norm = fold_rows(norms_y, total_f)
    nz_send[...] = tile(row_norm, row_decay, row_top)
    nz_buf[z] = nz_send[...]
    send_all(N2, "z", lambda p: nz_send, nz_buf)
    pre_top, pre_decay, pre_f = chain(
        decays_y, tops_y, empty, [included(i, y, False) for i in range(SIDE)]
    )
    pre_norm = fold_rows(norms_y, pre_f)

    recv_all(M1, "y", m_buf)
    sums = fold_tiles(m_buf, total_f, False, (zero_tile, zero_tile), None)
    mz_send[0] = sums[0]
    mz_send[1] = sums[1]
    mz_buf[z] = mz_send[...]
    send_all(M2, "z", lambda p: mz_send, mz_buf)

    recv_all(N2, "z", nz_buf)
    tiles_z = [nz_buf[i] for i in range(SIDE)]
    els = [element(tiles_z, i, False, (0, 1, 2)) for i in range(SIDE)]
    norms_z, decays_z, tops_z = zip(*els)
    far_top, unused, far_f = chain(
        decays_z, tops_z, empty, [included(i, z, False) for i in range(SIDE)]
    )
    far_norm = fold_rows(norms_z, far_f)
    in_top = jnp.maximum(far_top + pre_decay, pre_top)
    in_norm = jnp.exp(far_top + pre_decay - in_top) * far_norm + jnp.exp(pre_top - in_top) * pre_norm

    query2 = jnp.concatenate([q_ref[...], q_ref[...]], axis=1).astype(F32)
    qn = half_sum(query2 * in_norm)
    in_tops = both(in_top)
    alpha, beta, inv, den, big, back, back_top = [], [], [], [], [], [], []
    for d in range(2):
        carry = c_col[d] + in_tops[d]
        m = jnp.maximum(carry, m_local[d])
        a = jnp.exp(m_local[d] - m)
        b = jnp.exp(carry - m)
        dn = b * qn[d] + a * den_local[d]
        floor = jnp.exp(-m)
        size = jnp.abs(dn)
        blog = c_col[d] - m
        peak = jnp.max(blog, axis=0, keepdims=True)
        alpha.append(a)
        beta.append(b)
        den.append(dn)
        big.append(size > floor)
        inv.append(1.0 / jnp.maximum(size, floor))
        back_top.append(peak)
        back.append(jnp.exp(blog - peak))
    back2 = pack(back_top[0], back_top[1])
    slope = dot_left(query2 * pack(back[0] * inv[0], back[1] * inv[1]), g_ref[...], 0, 0)
    g_send[:, 0] = slope[:DK].reshape(SIDE, 8, DV)
    g_send[:, 1] = slope[DK:].reshape(SIDE, 8, DV)
    g_send[:, 2] = jnp.broadcast_to(tile(back2, back2, back2), (SIDE, 8, DV))
    g_buf[y] = g_send[y]
    send_all(G1, "y", lambda p: g_send.at[p], g_buf)

    unused, unused, into_f = chain(decays_y, tops_y, far_top, None)
    recv_all(M2, "z", mz_buf)
    far = fold_tiles(mz_buf, far_f, False, (zero_tile, zero_tile), None)
    fold_tiles(m_buf, into_f, False, far, mr_send)
    mr_buf[y] = mr_send[y]
    send_all(M3, "y", lambda p: mr_send.at[p], mr_buf)

    u_s[...] = (w_s[0] * (alpha[0] * inv[0]) + w_s[1] * (alpha[1] * inv[1])) * s_s[...]
    v_local = dot_left(u_s[...], g_ref[...], 0, 0)

    recv_all(G1, "y", g_buf)
    els = [
        jnp.where(first, g_buf[SIDE - 1 - i, 2, 0:1], g_buf[i, 2, 0:1]) for i in range(SIDE)
    ]
    back_decays_y = decays_y[::-1]
    g_top, unused, g_total_f = chain(back_decays_y, els, empty, None)
    back_y = els
    sums = fold_tiles(g_buf, g_total_f, True, (zero_tile, zero_tile), None)
    gz_send[0] = sums[0]
    gz_send[1] = sums[1]
    gz_send[2] = tile(g_top, g_top, g_top)
    gz_buf[z] = gz_send[...]
    send_all(G2, "z", lambda p: gz_send, gz_buf)
    g_pre_top, g_pre_decay, g_pre_f = chain(
        back_decays_y, back_y, empty, [included(i, y, True) for i in range(SIDE)]
    )

    recv_all(M3, "y", mr_buf)
    in_mem = jnp.concatenate(
        [mr_buf[:, 0].reshape(DK, DV), mr_buf[:, 1].reshape(DK, DV)], axis=0
    )
    cross = dot_right(g_ref[...], in_mem, 1, 1)
    gq = half_sum(query2 * cross)
    gd, row_total = [], []
    for d in range(2):
        along = (beta[d] * gq[d] + alpha[d] * num_local[d]) * inv[d]
        signed = jnp.where(den[d] > 0.0, -along, along) * inv[d]
        gd.append(jnp.where(big[d], signed, 0.0))
        row_total.append(jnp.where(big[d], 0.0, along))
    n_grad = jnp.sum(query2 * pack(back[0] * gd[0], back[1] * gd[1]), axis=0, keepdims=True)
    h_send[...] = jnp.broadcast_to(n_grad, (8, DV))
    h_buf[y] = h_send[...]
    send_all(H1, "y", lambda p: h_send, h_buf)

    recv_all(G2, "z", gz_buf)
    back_decays_z = decays_z[::-1]
    back_z = [
        jnp.where(first, gz_buf[SIDE - 1 - i, 2, 0:1], gz_buf[i, 2, 0:1]) for i in range(SIDE)
    ]
    g_far_top, unused, g_far_f = chain(
        back_decays_z, back_z, empty, [included(i, z, True) for i in range(SIDE)]
    )
    far = fold_tiles(gz_buf, g_far_f, True, (zero_tile, zero_tile), None)
    unused, unused, g_into_f = chain(back_decays_y, back_y, g_far_top, None)
    fold_tiles(g_buf, g_into_f, True, far, gr_send)
    gr_buf[y] = gr_send[y]
    send_all(G3, "y", lambda p: gr_send.at[p], gr_buf)

    recv_all(H1, "y", h_buf)
    n_rows_y = [jnp.where(first, h_buf[SIDE - 1 - i, 0:1], h_buf[i, 0:1]) for i in range(SIDE)]
    hz_send[...] = jnp.broadcast_to(fold_rows(n_rows_y, g_total_f), (8, DV))
    hz_buf[z] = hz_send[...]
    send_all(H2, "z", lambda p: hz_send, hz_buf)
    g_pre_norm = fold_rows(n_rows_y, g_pre_f)

    column_sum = []
    for d in range(2):
        part = w_s[d] * (r_s[...] * (alpha[d] * inv[d]) + alpha[d] * gd[d])
        if d == 0:
            p_s[...] = part
        else:
            p_s[...] += part
        column_sum.append(jnp.sum(part * s_s[...], axis=0, keepdims=True))
    p_high, p_low = halves(p_s[...])
    gq_local = dot(p_high, k_ref[...], 1, 0) + dot(p_low, k_ref[...], 1, 0)
    k_local = dot(p_high, q_ref[...], 0, 0) + dot(p_low, q_ref[...], 0, 0)
    carried = cross * pack(beta[0] * inv[0], beta[1] * inv[1]) + in_norm * pack(
        beta[0] * gd[0], beta[1] * gd[1]
    )
    gq_out[...] = (gq_local + carried[:, :DK] + carried[:, DK:]).astype(BF16)

    for j in range(SIDE):
        ft[j] = f_ref[:, j * TOK : (j + 1) * TOK].T

    for i in range(1, 4):
        p = lax.rem(x + i, 4) * 2 + core
        copy(VX, "tp", p, vw_ref, vall.at[p], p).wait_recv()
        pltpu.make_async_remote_copy(
            src_ref=vall.at[p], dst_ref=vall.at[p], send_sem=ssem.at[VC, p],
            recv_sem=rsem.at[VC, p], device_id=peer_id("tp", mate), device_id_type=MESH,
        ).start()

    g_in_top = jnp.maximum(g_far_top + g_pre_decay, g_pre_top)
    g_tops = both(g_in_top)
    scale2 = pack(jnp.exp(ending[0] + g_tops[0]), jnp.exp(ending[1] + g_tops[1]))
    scaled = key2 * scale2
    recv_all(G3, "y", gr_buf)
    in_slope = jnp.concatenate(
        [gr_buf[:, 0].reshape(DK, DV), gr_buf[:, 1].reshape(DK, DV)], axis=0
    )
    slope_high, slope_low = halves(in_slope)
    scaled_high, scaled_low = halves(scaled)
    grad_values = (
        v_local
        + dot(scaled_high, slope_high, 1, 0)
        + dot(scaled_high, slope_low, 1, 0)
        + dot(scaled_low, slope_high, 1, 0)
    ).astype(BF16)
    gv_s[...] = grad_values.reshape(N_TP, TOK // N_TP, DV)
    gv_buf[tp] = gv_s[tp]
    send_all(GV, "tp", lambda p: gv_s.at[p], gv_buf)

    gv_all = gv_s[...].reshape(TOK, DV)
    for i in range(1, SIDE + 1):
        p = lax.rem(z + i, SIDE)
        piece = dot(ft[p], gv_all, 1, 0).astype(BF16).reshape(SIDE, 2, ROWS // 2, DV)
        wa_send[p] = piece[:, 0]
        wb_send[:, p] = piece[:, 1]
        if i < SIDE:
            copy(A1, "z", p, wa_send.at[p], wa_buf.at[z], z).start()
    wa_buf[z] = wa_send[z]
    wb_buf[y] = wb_send[y]
    send_all(B1, "y", lambda p: wb_send.at[p], wb_buf)

    recv_all(H2, "z", hz_buf)
    n_rows_z = [jnp.where(first, hz_buf[SIDE - 1 - i, 0:1], hz_buf[i, 0:1]) for i in range(SIDE)]
    g_far_norm = fold_rows(n_rows_z, g_far_f)
    g_in_norm = (
        jnp.exp(g_far_top + g_pre_decay - g_in_top) * g_far_norm
        + jnp.exp(g_pre_top - g_in_top) * g_pre_norm
    )
    values = v_s[...]
    passed = dot(values, slope_high, 1, 1) + dot(values, slope_low, 1, 1) + g_in_norm
    moved = scale2 * passed
    gk_out[...] = (k_local + moved[:, :DK] + moved[:, DK:]).astype(BF16)
    carried_column = half_sum(scaled * passed)
    pair = in_mem * in_slope
    pair_norm = half_sum(in_norm * g_in_norm)
    for d in range(2):
        gi_out[d] = column_sum[d] + row_of(carried_column[d])
        inner = jnp.sum(
            jnp.sum(pair[d * DK : (d + 1) * DK], axis=0, keepdims=True), axis=1, keepdims=True
        )
        across = jnp.exp(in_tops[d] + decay[d] + g_tops[d]) * (inner + pair_norm[d])
        ahead = row_total[d] - column(column_sum[d])
        span = jnp.where(reach[d], ahead, carried_column[d])
        gf_out[d] = jnp.sum(span, axis=0, keepdims=True) + across

    place.wait()
    for j in range(4):
        p = j * 2 + (1 - core)
        copy(VC, "tp", p, vw_ref, vall.at[p], p).wait_recv()
    recv_all(GV, "tp", gv_buf)
    for j in range(4):
        cols = slice(j * 512, (j + 1) * 512)
        acc = dot(gv_buf[0], vall[0, cols], 1, 1)
        for h in range(1, N_TP):
            acc += dot(gv_buf[h], vall[h, cols], 1, 1)
        gx_out[:, cols] = acc.astype(BF16)

    recv_all(A1, "z", wa_buf)
    wa2_send[...] = jnp.sum(wa_buf[...].astype(F32), axis=0).astype(BF16)
    wa2_buf[y] = wa2_send[y]
    send_all(A2, "y", lambda p: wa2_send.at[p], wa2_buf)
    recv_all(B1, "y", wb_buf)
    wb2_send[...] = jnp.sum(wb_buf[...].astype(F32), axis=0).astype(BF16)
    wb2_buf[z] = wb2_send[z]
    send_all(B2, "z", lambda p: wb2_send.at[p], wb2_buf)
    recv_all(A2, "y", wa2_buf)
    gw_out[: ROWS // 2] = jnp.sum(wa2_buf[...].astype(F32), axis=0)
    recv_all(B2, "z", wb2_buf)
    gw_out[ROWS // 2 :] = jnp.sum(wb2_buf[...].astype(F32), axis=0)

    for kind, axis, src_of, buf in (
        (N1, "y", lambda p: n_send, n_buf),
        (N2, "z", lambda p: nz_send, nz_buf),
        (M1, "y", lambda p: m_send.at[p], m_buf),
        (M2, "z", lambda p: mz_send, mz_buf),
        (M3, "y", lambda p: mr_send.at[p], mr_buf),
        (G1, "y", lambda p: g_send.at[p], g_buf),
        (G2, "z", lambda p: gz_send, gz_buf),
        (G3, "y", lambda p: gr_send.at[p], gr_buf),
        (H1, "y", lambda p: h_send, h_buf),
        (H2, "z", lambda p: hz_send, hz_buf),
        (A1, "z", lambda p: wa_send.at[p], wa_buf),
        (B1, "y", lambda p: wb_send.at[p], wb_buf),
        (A2, "y", lambda p: wa2_send.at[p], wa2_buf),
        (B2, "z", lambda p: wb2_send.at[p], wb2_buf),
        (GV, "tp", lambda p: gv_s.at[p], gv_buf),
    ):
        sent_all(kind, axis, src_of, buf)
    for i in range(1, 4):
        p = lax.rem(x + i, 4) * 2 + core
        copy(VX, "tp", p, vw_ref, vall.at[tp], tp).wait_send()
        copy(VC, "tp", p, vall.at[p], vall.at[p], p).wait_send()
    copy(VC, "tp", mate, vw_ref, vall.at[tp], tp).wait_send()


def body(features, value_weight, queries, key_vectors, log_input, log_forget, out_grad):
    whole = pl.BlockSpec(memory_space=pltpu.VMEM)
    tile = (8, DV)
    part = (ROWS // 2, DV)
    scratch = [
        pltpu.VMEM((TOK, DV), BF16),
        pltpu.VMEM((SIDE, TOK, TOK), BF16),
        pltpu.VMEM((2, TOK, TOK), F32),
        pltpu.VMEM((TOK, TOK), F32),
        pltpu.VMEM((TOK, TOK), F32),
        pltpu.VMEM((TOK, TOK), F32),
        pltpu.VMEM((TOK, TOK), F32),
        pltpu.VMEM(tile, F32),
        pltpu.VMEM((SIDE, *tile), F32),
        pltpu.VMEM(tile, F32),
        pltpu.VMEM((SIDE, *tile), F32),
        pltpu.VMEM((SIDE, 2, *tile), F32),
        pltpu.VMEM((SIDE, 2, *tile), F32),
        pltpu.VMEM((2, *tile), F32),
        pltpu.VMEM((SIDE, 2, *tile), F32),
        pltpu.VMEM((SIDE, 2, *tile), F32),
        pltpu.VMEM((SIDE, 2, *tile), F32),
        pltpu.VMEM((SIDE, 3, *tile), F32),
        pltpu.VMEM((SIDE, 3, *tile), F32),
        pltpu.VMEM((3, *tile), F32),
        pltpu.VMEM((SIDE, 3, *tile), F32),
        pltpu.VMEM((SIDE, 2, *tile), F32),
        pltpu.VMEM((SIDE, 2, *tile), F32),
        pltpu.VMEM(tile, F32),
        pltpu.VMEM((SIDE, *tile), F32),
        pltpu.VMEM(tile, F32),
        pltpu.VMEM((SIDE, *tile), F32),
        pltpu.VMEM((SIDE, SIDE, *part), BF16),
        pltpu.VMEM((SIDE, SIDE, *part), BF16),
        pltpu.VMEM((SIDE, SIDE, *part), BF16),
        pltpu.VMEM((SIDE, SIDE, *part), BF16),
        pltpu.VMEM((SIDE, *part), BF16),
        pltpu.VMEM((SIDE, *part), BF16),
        pltpu.VMEM((SIDE, *part), BF16),
        pltpu.VMEM((SIDE, *part), BF16),
        pltpu.VMEM((N_TP, D, DV), BF16),
        pltpu.VMEM((N_TP, TOK // N_TP, DV), BF16),
        pltpu.VMEM((N_TP, TOK // N_TP, DV), BF16),
        pltpu.SemaphoreType.DMA((KINDS, SIDE)),
        pltpu.SemaphoreType.DMA((KINDS, SIDE)),
        pltpu.SemaphoreType.DMA,
    ]
    return pl.pallas_call(
        kernel,
        out_shape=(
            jax.ShapeDtypeStruct((TOK, DK), BF16),
            jax.ShapeDtypeStruct((TOK, DK), BF16),
            jax.ShapeDtypeStruct((2, 1, TOK), F32),
            jax.ShapeDtypeStruct((2, 1, TOK), F32),
            jax.ShapeDtypeStruct((ROWS, DV), F32),
            jax.ShapeDtypeStruct((TOK // N_TP, D), BF16),
        ),
        in_specs=[whole] * 7,
        out_specs=[whole] * 6,
        scratch_shapes=scratch,
        compiler_params=pltpu.CompilerParams(
            collective_id=0, has_side_effects=True, vmem_limit_bytes=48 * 1024 * 1024
        ),
    )(features, value_weight, queries, key_vectors, log_input, log_forget, out_grad)


def solution(mesh):
    placed = (
        P("sp", None),
        P(None, "tp"),
        P("sp", "tp"),
        P("sp", "tp"),
        P(None, "tp", "sp"),
        P(None, "tp", "sp"),
        P("sp", "tp"),
    )
    return jax.shard_map(
        body,
        mesh=mesh,
        in_specs=placed,
        out_specs=(
            P("sp", "tp"),
            P("sp", "tp"),
            P(None, "tp", "sp"),
            P(None, "tp", "sp"),
            P("sp", "tp"),
            P(("sp", "tp"), None),
        ),
        check_vma=False,
    )
```

```python
import jax
import jax.numpy as jnp
from jax import lax
from jax.experimental import pallas as pl
from jax.experimental.pallas import tpu as pltpu
from jax.sharding import PartitionSpec as P

DK = 64
DV = 128
TOK = 256
D = 2048
SIDE = 8
N_TP = 8
ROWS = D // 64

LOW = -1e30
F32 = jnp.float32
BF16 = jnp.bfloat16
MESH = pl.DeviceIdType.MESH

(N1, N2, M1, M2, M3, G1, G2, G3, H1, H2, A1, B1, A2, B2, GV, VL, VR, VA, VB, C0, C1, C2, C3, KINDS) = range(24)
FAR_FIRST = (4, 3, 5, 2, 6, 1, 7)
HALF = D // 2


def dot(a, b, da, db):
    return lax.dot_general(a, b, (((da,), (db,)), ((), ())), preferred_element_type=F32)


def halves(x):
    high = x.astype(BF16)
    return high, (x - high.astype(F32)).astype(BF16)


def dot_left(x, b, da, db):
    high, low = halves(x)
    return dot(high, b, da, db) + dot(low, b, da, db)


def dot_right(a, x, da, db):
    high, low = halves(x)
    return dot(a, high, da, db) + dot(a, low, da, db)


def kernel(
    f_in, vw_in, q_in, k_in, li_in, lf_in, g_in,
    gq_out, gk_out, gi_out, gf_out, gw_out, gx_out,
    f_ref, q_ref, k_ref, li_ref, lf_ref, g_ref,
    v_s, ft, w_s, s_s, r_s, p_s, u_s,
    n_send, n_buf, nz_send, nz_buf,
    m_send, m_buf, mz_send, mz_buf, mr_send, mr_buf,
    g_send, g_buf, gz_send, gz_buf, gr_send, gr_buf,
    h_send, h_buf, hz_send, hz_buf,
    wa_send, wa_buf, wb_send, wb_buf, wa2_send, wa2_buf, wb2_send, wb2_buf,
    vall, gv_s, gv_buf, ssem, rsem, lsem,
):
    sp = lax.axis_index("sp")
    tp = lax.axis_index("tp")
    z, y = lax.div(sp, SIDE), lax.rem(sp, SIDE)
    x, core = lax.div(tp, 2), lax.rem(tp, 2)

    loads = [
        pltpu.make_async_copy(src, dst, lsem.at[n])
        for n, (src, dst) in enumerate(
            (
                (lf_in, lf_ref), (li_in, li_ref), (vw_in, vall.at[tp]), (f_in, f_ref),
                (k_in, k_ref), (q_in, q_ref), (g_in, g_ref),
            )
        )
    ]
    for load in loads:
        load.start()

    def peer_id(axis, p):
        if axis == "y":
            return {"sp": z * SIDE + p}
        if axis == "z":
            return {"sp": p * SIDE + y}
        return {"tp": p}

    own = {"y": y, "z": z, "tp": tp}

    def copy(kind, axis, p, src, dst):
        return pltpu.make_async_remote_copy(
            src_ref=src, dst_ref=dst, send_sem=ssem.at[kind], recv_sem=rsem.at[kind],
            device_id=peer_id(axis, p), device_id_type=MESH,
        )

    def send_all(kind, axis, src_of, buf):
        me = own[axis]
        for i in FAR_FIRST:
            p = lax.rem(me + i, SIDE)
            copy(kind, axis, p, src_of(p), buf.at[me]).start()

    def all_of(kind, axis, buf):
        rest = buf.at[pl.ds(0, SIDE - 1)]
        return copy(kind, axis, lax.rem(own[axis] + 1, SIDE), rest, rest)

    def recv_all(kind, axis, buf):
        all_of(kind, axis, buf).wait_recv()

    def sent_all(kind, axis, buf):
        all_of(kind, axis, buf).wait_send()

    barrier = pltpu.get_barrier_semaphore()
    for axis in ("y", "z", "tp"):
        for i in FAR_FIRST:
            p = lax.rem(own[axis] + i, SIDE)
            pl.semaphore_signal(barrier, inc=1, device_id=peer_id(axis, p), device_id_type=MESH)

    loads[0].wait()
    loads[1].wait()
    at_t = lax.broadcasted_iota(jnp.int32, (TOK, TOK), 0)
    at_s = lax.broadcasted_iota(jnp.int32, (TOK, TOK), 1)
    same = at_t == at_s
    reach = (at_s <= at_t, at_s >= at_t)
    lane = lax.broadcasted_iota(jnp.int32, (1, 2 * DK), 1)
    first = lane < DK
    sub = lax.broadcasted_iota(jnp.int32, (8, 2 * DK), 0)

    def column(row):
        return jnp.sum(jnp.where(same, row, 0.0), axis=1, keepdims=True)

    def row_of(col):
        return jnp.sum(jnp.where(same, col, 0.0), axis=0, keepdims=True)

    def pack(a, b):
        return jnp.where(first, a, b)

    def half_sum(packed):
        return (
            jnp.sum(jnp.where(first, packed, 0.0), axis=1, keepdims=True),
            jnp.sum(jnp.where(first, 0.0, packed), axis=1, keepdims=True),
        )

    c_col, i_row, c_row, end, ending, decay, top = [], [], [], [], [], [], []
    for d in range(2):
        l_row = lf_ref[d]
        in_row = li_ref[d]
        c = jnp.sum(jnp.where(reach[d], l_row, 0.0), axis=1, keepdims=True)
        cr = row_of(c)
        total = c[TOK - 1 :, :] if d == 0 else c[:1, :]
        e = total - c + column(in_row)
        peak = jnp.max(e, axis=0, keepdims=True)
        c_col.append(c)
        c_row.append(cr)
        i_row.append(in_row)
        ending.append(e)
        decay.append(total)
        top.append(peak)
    loads[4].wait()
    key2 = jnp.concatenate([k_ref[...], k_ref[...]], axis=0).astype(F32).T
    key = key2[:, :DK].astype(BF16)
    weighted = key2 * pack(jnp.exp(ending[0] - top[0]), jnp.exp(ending[1] - top[1]))
    norm = jnp.sum(weighted, axis=0, keepdims=True)
    decay2 = pack(decay[0], decay[1])
    top2 = pack(top[0], top[1])

    def tile(a, b, c):
        return jnp.where(sub == 0, a, jnp.where(sub == 1, b, jnp.where(sub == 2, c, 0.0)))

    n_send[...] = tile(norm, decay2, top2)
    n_buf[y] = n_send[...]
    loads[2].wait()
    loads[3].wait()
    values = jnp.dot(f_ref[...], vall[tp], preferred_element_type=F32).astype(BF16)
    v_s[...] = values
    pl.semaphore_wait(barrier, 3 * (SIDE - 1))
    send_all(N1, "y", lambda p: n_send, n_buf)

    memory = dot_left(weighted, values, 0, 0)
    m_send[:, 0] = memory[:DK].reshape(SIDE, 8, DV)
    m_send[:, 1] = memory[DK:].reshape(SIDE, 8, DV)
    m_buf[y] = m_send[y]
    send_all(M1, "y", lambda p: m_send.at[p], m_buf)

    mate = x * 2 + (1 - core)
    left = lax.rem(x + 3, 4) * 2 + core
    right = lax.rem(x + 1, 4) * 2 + core
    across_x = lax.rem(x + 2, 4) * 2 + core
    mine = vall.at[tp]
    copy(VL, "tp", right, mine, mine).start()
    copy(VR, "tp", left, mine, mine).start()
    copy(C0, "tp", mate, mine, mine).start()

    loads[5].wait()
    loads[6].wait()
    query2 = jnp.concatenate([q_ref[...], q_ref[...]], axis=0).astype(F32).T
    s_s[...] = dot(q_ref[...], k_ref[...], 0, 0)
    r_s[...] = dot(g_ref[...], v_s[...], 1, 1)
    m_local, den_local, num_local = [], [], []
    for d in range(2):
        e = jnp.where(reach[d], c_col[d] - c_row[d] + i_row[d], LOW)
        peak = jnp.max(e, axis=1, keepdims=True)
        w = jnp.exp(e - peak)
        w_s[d] = w
        ws = w * s_s[...]
        m_local.append(peak)
        den_local.append(jnp.sum(ws, axis=1, keepdims=True))
        num_local.append(jnp.sum(ws * r_s[...], axis=1, keepdims=True))

    def element(tiles, i, flip, rows):
        near, far = tiles[i], tiles[SIDE - 1 - i]
        take = first if not flip else jnp.logical_not(first)
        return [jnp.where(take, near[r : r + 1], far[r : r + 1]) for r in rows]

    def included(i, at, flip):
        low = jnp.where(i < at, 1, 0)
        high = jnp.where(SIDE - 1 - i > at, 1, 0)
        if flip:
            low, high = high, low
        return jnp.where(first, low, high) > 0

    empty = jnp.full((1, 2 * DK), LOW, F32)

    def chain(decays, tops, start, masks):
        run, past, factors = start, jnp.zeros((1, 2 * DK), F32), []
        for i in range(SIDE):
            dec, high = decays[i], tops[i]
            if masks is not None:
                dec = jnp.where(masks[i], dec, 0.0)
                high = jnp.where(masks[i], high, LOW)
            new = jnp.maximum(run + dec, high)
            keep = jnp.exp(run + dec - new)
            add = jnp.exp(high - new)
            if masks is not None:
                add = jnp.where(masks[i], add, 0.0)
            factors.append((keep, add))
            run, past = new, past + dec
        return run, past, factors

    def fold_rows(rows, factors):
        acc = jnp.zeros((1, 2 * DK), F32)
        for row, (keep, add) in zip(rows, factors):
            acc = keep * acc + add * row
        return acc

    def both(factor):
        return factor[:, :1], factor[:, DK : DK + 1]

    def fold_tiles(buf, factors, flip, start, store):
        acc = list(start)
        for i in range(SIDE):
            keep, add = both(factors[i][0]), both(factors[i][1])
            places = (i, SIDE - 1 - i) if not flip else (SIDE - 1 - i, i)
            for d in range(2):
                if store is not None:
                    store[places[d], d] = acc[d]
                acc[d] = keep[d] * acc[d] + add[d] * buf[places[d], d]
        return acc

    zero_tile = jnp.zeros((8, DV), F32)

    recv_all(N1, "y", n_buf)
    tiles_y = [n_buf[i] for i in range(SIDE)]
    els = [element(tiles_y, i, False, (0, 1, 2)) for i in range(SIDE)]
    norms_y, decays_y, tops_y = zip(*els)
    row_top, row_decay, total_f = chain(decays_y, tops_y, empty, None)
    row_norm = fold_rows(norms_y, total_f)
    nz_send[...] = tile(row_norm, row_decay, row_top)
    nz_buf[z] = nz_send[...]
    send_all(N2, "z", lambda p: nz_send, nz_buf)
    pre_top, pre_decay, pre_f = chain(
        decays_y, tops_y, empty, [included(i, y, False) for i in range(SIDE)]
    )
    pre_norm = fold_rows(norms_y, pre_f)

    recv_all(M1, "y", m_buf)
    sums = fold_tiles(m_buf, total_f, False, (zero_tile, zero_tile), None)
    mz_send[0] = sums[0]
    mz_send[1] = sums[1]
    mz_buf[z] = mz_send[...]
    send_all(M2, "z", lambda p: mz_send, mz_buf)

    recv_all(N2, "z", nz_buf)
    tiles_z = [nz_buf[i] for i in range(SIDE)]
    els = [element(tiles_z, i, False, (0, 1, 2)) for i in range(SIDE)]
    norms_z, decays_z, tops_z = zip(*els)
    far_top, unused, far_f = chain(
        decays_z, tops_z, empty, [included(i, z, False) for i in range(SIDE)]
    )
    far_norm = fold_rows(norms_z, far_f)
    in_top = jnp.maximum(far_top + pre_decay, pre_top)
    in_norm = jnp.exp(far_top + pre_decay - in_top) * far_norm + jnp.exp(pre_top - in_top) * pre_norm

    qn = half_sum(query2 * in_norm)
    in_tops = both(in_top)
    alpha, beta, inv, den, big, back, back_top = [], [], [], [], [], [], []
    for d in range(2):
        carry = c_col[d] + in_tops[d]
        m = jnp.maximum(carry, m_local[d])
        a = jnp.exp(m_local[d] - m)
        b = jnp.exp(carry - m)
        dn = b * qn[d] + a * den_local[d]
        floor = jnp.exp(-m)
        size = jnp.abs(dn)
        blog = c_col[d] - m
        peak = jnp.max(blog, axis=0, keepdims=True)
        alpha.append(a)
        beta.append(b)
        den.append(dn)
        big.append(size > floor)
        inv.append(1.0 / jnp.maximum(size, floor))
        back_top.append(peak)
        back.append(jnp.exp(blog - peak))
    back2 = pack(back_top[0], back_top[1])
    slope = dot_left(query2 * pack(back[0] * inv[0], back[1] * inv[1]), g_ref[...], 0, 0)
    g_send[:, 0] = slope[:DK].reshape(SIDE, 8, DV)
    g_send[:, 1] = slope[DK:].reshape(SIDE, 8, DV)
    g_send[:, 2] = jnp.broadcast_to(tile(back2, back2, back2), (SIDE, 8, DV))
    g_buf[y] = g_send[y]
    send_all(G1, "y", lambda p: g_send.at[p], g_buf)

    unused, unused, into_f = chain(decays_y, tops_y, far_top, None)
    recv_all(M2, "z", mz_buf)
    far = fold_tiles(mz_buf, far_f, False, (zero_tile, zero_tile), None)
    fold_tiles(m_buf, into_f, False, far, mr_send)
    mr_buf[y] = mr_send[y]
    send_all(M3, "y", lambda p: mr_send.at[p], mr_buf)

    u_s[...] = (w_s[0] * (alpha[0] * inv[0]) + w_s[1] * (alpha[1] * inv[1])) * s_s[...]
    v_local = dot_left(u_s[...], g_ref[...], 0, 0)

    from_left, from_right = vall.at[left], vall.at[right]
    copy(VL, "tp", left, mine, from_left).wait_recv()
    part = vall.at[left, pl.ds(0, HALF)]
    copy(VA, "tp", right, part, part).start()
    copy(C1, "tp", mate, from_left, from_left).start()
    copy(VR, "tp", right, mine, from_right).wait_recv()
    part = vall.at[right, pl.ds(HALF, HALF)]
    copy(VB, "tp", left, part, part).start()
    copy(C2, "tp", mate, from_right, from_right).start()

    recv_all(G1, "y", g_buf)
    els = [
        jnp.where(first, g_buf[SIDE - 1 - i, 2, 0:1], g_buf[i, 2, 0:1]) for i in range(SIDE)
    ]
    back_decays_y = decays_y[::-1]
    g_top, unused, g_total_f = chain(back_decays_y, els, empty, None)
    back_y = els
    sums = fold_tiles(g_buf, g_total_f, True, (zero_tile, zero_tile), None)
    gz_send[0] = sums[0]
    gz_send[1] = sums[1]
    gz_send[2] = tile(g_top, g_top, g_top)
    gz_buf[z] = gz_send[...]
    send_all(G2, "z", lambda p: gz_send, gz_buf)
    g_pre_top, g_pre_decay, g_pre_f = chain(
        back_decays_y, back_y, empty, [included(i, y, True) for i in range(SIDE)]
    )

    recv_all(M3, "y", mr_buf)
    in_mem = jnp.concatenate(
        [mr_buf[:, 0].reshape(DK, DV), mr_buf[:, 1].reshape(DK, DV)], axis=0
    )
    cross = dot_right(g_ref[...], in_mem, 1, 1)
    gq = half_sum(query2 * cross)
    gd, row_total = [], []
    for d in range(2):
        along = (beta[d] * gq[d] + alpha[d] * num_local[d]) * inv[d]
        signed = jnp.where(den[d] > 0.0, -along, along) * inv[d]
        gd.append(jnp.where(big[d], signed, 0.0))
        row_total.append(jnp.where(big[d], 0.0, along))
    n_grad = jnp.sum(query2 * pack(back[0] * gd[0], back[1] * gd[1]), axis=0, keepdims=True)
    h_send[...] = jnp.broadcast_to(n_grad, (8, DV))
    h_buf[y] = h_send[...]
    send_all(H1, "y", lambda p: h_send, h_buf)

    recv_all(G2, "z", gz_buf)
    back_decays_z = decays_z[::-1]
    back_z = [
        jnp.where(first, gz_buf[SIDE - 1 - i, 2, 0:1], gz_buf[i, 2, 0:1]) for i in range(SIDE)
    ]
    g_far_top, unused, g_far_f = chain(
        back_decays_z, back_z, empty, [included(i, z, True) for i in range(SIDE)]
    )
    far = fold_tiles(gz_buf, g_far_f, True, (zero_tile, zero_tile), None)
    unused, unused, g_into_f = chain(back_decays_y, back_y, g_far_top, None)
    fold_tiles(g_buf, g_into_f, True, far, gr_send)
    gr_buf[y] = gr_send[y]
    send_all(G3, "y", lambda p: gr_send.at[p], gr_buf)

    recv_all(H1, "y", h_buf)
    n_rows_y = [jnp.where(first, h_buf[SIDE - 1 - i, 0:1], h_buf[i, 0:1]) for i in range(SIDE)]
    hz_send[...] = jnp.broadcast_to(fold_rows(n_rows_y, g_total_f), (8, DV))
    hz_buf[z] = hz_send[...]
    send_all(H2, "z", lambda p: hz_send, hz_buf)
    g_pre_norm = fold_rows(n_rows_y, g_pre_f)

    column_sum = []
    for d in range(2):
        part = w_s[d] * (r_s[...] * (alpha[d] * inv[d]) + alpha[d] * gd[d])
        if d == 0:
            p_s[...] = part
        else:
            p_s[...] += part
        column_sum.append(jnp.sum(part * s_s[...], axis=0, keepdims=True))
    p_high, p_low = halves(p_s[...])
    gq_local = dot(k_ref[...], p_high, 1, 1) + dot(k_ref[...], p_low, 1, 1)
    k_local = dot(q_ref[...], p_high, 1, 0) + dot(q_ref[...], p_low, 1, 0)
    carried = cross * pack(beta[0] * inv[0], beta[1] * inv[1]) + in_norm * pack(
        beta[0] * gd[0], beta[1] * gd[1]
    )
    turned = carried.T
    gq_out[...] = (gq_local + turned[:DK] + turned[DK:]).astype(BF16)

    for j in range(SIDE):
        ft[j] = f_ref[:, j * TOK : (j + 1) * TOK].T

    opposite = vall.at[across_x]
    copy(VA, "tp", left, vall.at[tp, pl.ds(0, HALF)], vall.at[across_x, pl.ds(0, HALF)]).wait_recv()
    copy(VB, "tp", left, vall.at[tp, pl.ds(0, HALF)], vall.at[across_x, pl.ds(HALF, HALF)]).wait_recv()
    copy(C3, "tp", mate, opposite, opposite).start()

    g_in_top = jnp.maximum(g_far_top + g_pre_decay, g_pre_top)
    g_tops = both(g_in_top)
    scale2 = pack(jnp.exp(ending[0] + g_tops[0]), jnp.exp(ending[1] + g_tops[1]))
    scaled = key2 * scale2
    recv_all(G3, "y", gr_buf)
    in_slope = jnp.concatenate(
        [gr_buf[:, 0].reshape(DK, DV), gr_buf[:, 1].reshape(DK, DV)], axis=0
    )
    slope_high, slope_low = halves(in_slope)
    scaled_high, scaled_low = halves(scaled)
    grad_values = (
        v_local
        + dot(scaled_high, slope_high, 1, 0)
        + dot(scaled_high, slope_low, 1, 0)
        + dot(scaled_low, slope_high, 1, 0)
    ).astype(BF16)
    gv_s[...] = grad_values.reshape(N_TP, TOK // N_TP, DV)
    gv_buf[tp] = gv_s[tp]
    send_all(GV, "tp", lambda p: gv_s.at[p], gv_buf)

    gv_all = gv_s[...].reshape(TOK, DV)
    for i in range(1, SIDE + 1):
        p = lax.rem(z + i, SIDE)
        piece = dot(ft[p], gv_all, 1, 0).astype(BF16).reshape(SIDE, 2, ROWS // 2, DV)
        wa_send[p] = piece[:, 0]
        wb_send[:, p] = piece[:, 1]
        if i < SIDE:
            copy(A1, "z", p, wa_send.at[p], wa_buf.at[z]).start()
    wa_buf[z] = wa_send[z]
    wb_buf[y] = wb_send[y]
    send_all(B1, "y", lambda p: wb_send.at[p], wb_buf)

    recv_all(H2, "z", hz_buf)
    n_rows_z = [jnp.where(first, hz_buf[SIDE - 1 - i, 0:1], hz_buf[i, 0:1]) for i in range(SIDE)]
    g_far_norm = fold_rows(n_rows_z, g_far_f)
    g_in_norm = (
        jnp.exp(g_far_top + g_pre_decay - g_in_top) * g_far_norm
        + jnp.exp(g_pre_top - g_in_top) * g_pre_norm
    )
    values = v_s[...]
    passed = dot(values, slope_high, 1, 1) + dot(values, slope_low, 1, 1) + g_in_norm
    moved = scale2 * passed
    turned = moved.T
    gk_out[...] = (k_local + turned[:DK] + turned[DK:]).astype(BF16)
    carried_column = half_sum(scaled * passed)
    pair = in_mem * in_slope
    pair_norm = half_sum(in_norm * g_in_norm)
    for d in range(2):
        gi_out[d] = column_sum[d] + row_of(carried_column[d])
        inner = jnp.sum(
            jnp.sum(pair[d * DK : (d + 1) * DK], axis=0, keepdims=True), axis=1, keepdims=True
        )
        across = jnp.exp(in_tops[d] + decay[d] + g_tops[d]) * (inner + pair_norm[d])
        ahead = row_total[d] - column(column_sum[d])
        span = jnp.where(reach[d], ahead, carried_column[d])
        gf_out[d] = jnp.sum(span, axis=0, keepdims=True) + across

    for kind in (C0, C1, C2, C3):
        copy(kind, "tp", mate, mine, vall.at[mate]).wait_recv()
    recv_all(GV, "tp", gv_buf)
    for j in range(4):
        cols = slice(j * 512, (j + 1) * 512)
        acc = dot(gv_buf[0], vall[0, cols], 1, 1)
        for h in range(1, N_TP):
            acc += dot(gv_buf[h], vall[h, cols], 1, 1)
        gx_out[:, cols] = acc.astype(BF16)

    recv_all(A1, "z", wa_buf)
    wa2_send[...] = jnp.sum(wa_buf[...].astype(F32), axis=0).astype(BF16)
    wa2_buf[y] = wa2_send[y]
    send_all(A2, "y", lambda p: wa2_send.at[p], wa2_buf)
    recv_all(B1, "y", wb_buf)
    wb2_send[...] = jnp.sum(wb_buf[...].astype(F32), axis=0).astype(BF16)
    wb2_buf[z] = wb2_send[z]
    send_all(B2, "z", lambda p: wb2_send.at[p], wb2_buf)
    recv_all(A2, "y", wa2_buf)
    gw_out[: ROWS // 2] = jnp.sum(wa2_buf[...].astype(F32), axis=0)
    recv_all(B2, "z", wb2_buf)
    gw_out[ROWS // 2 :] = jnp.sum(wb2_buf[...].astype(F32), axis=0)

    for kind, axis, buf in (
        (N1, "y", n_buf), (N2, "z", nz_buf), (M1, "y", m_buf), (M2, "z", mz_buf), (M3, "y", mr_buf),
        (G1, "y", g_buf), (G2, "z", gz_buf), (G3, "y", gr_buf), (H1, "y", h_buf), (H2, "z", hz_buf),
        (A1, "z", wa_buf), (B1, "y", wb_buf), (A2, "y", wa2_buf), (B2, "z", wb2_buf),
        (GV, "tp", gv_buf),
    ):
        sent_all(kind, axis, buf)
    for kind in (VL, VR, C0, C1, C2, C3):
        copy(kind, "tp", mate, mine, mine).wait_send()
    for kind in (VA, VB):
        part = vall.at[tp, pl.ds(0, HALF)]
        copy(kind, "tp", mate, part, part).wait_send()


def writer(*refs):
    srcs, dsts, sems = refs[:6], refs[6:12], refs[12]
    copies = [pltpu.make_async_copy(a, b, sems.at[n]) for n, (a, b) in enumerate(zip(srcs, dsts))]
    for c in copies:
        c.start()
    for c in copies:
        c.wait()


def body(features, value_weight, queries, key_vectors, log_input, log_forget, out_grad):
    whole = pl.BlockSpec(memory_space=pltpu.VMEM)
    outside = pl.BlockSpec(memory_space=pltpu.HBM)
    tile = (8, DV)
    part = (ROWS // 2, DV)
    scratch = [
        pltpu.VMEM((TOK, D), BF16),
        pltpu.VMEM((DK, TOK), BF16),
        pltpu.VMEM((DK, TOK), BF16),
        pltpu.VMEM((2, 1, TOK), F32),
        pltpu.VMEM((2, 1, TOK), F32),
        pltpu.VMEM((TOK, DV), BF16),
        pltpu.VMEM((TOK, DV), BF16),
        pltpu.VMEM((SIDE, TOK, TOK), BF16),
        pltpu.VMEM((2, TOK, TOK), F32),
        pltpu.VMEM((TOK, TOK), F32),
        pltpu.VMEM((TOK, TOK), F32),
        pltpu.VMEM((TOK, TOK), F32),
        pltpu.VMEM((TOK, TOK), F32),
        pltpu.VMEM(tile, F32),
        pltpu.VMEM((SIDE, *tile), F32),
        pltpu.VMEM(tile, F32),
        pltpu.VMEM((SIDE, *tile), F32),
        pltpu.VMEM((SIDE, 2, *tile), F32),
        pltpu.VMEM((SIDE, 2, *tile), F32),
        pltpu.VMEM((2, *tile), F32),
        pltpu.VMEM((SIDE, 2, *tile), F32),
        pltpu.VMEM((SIDE, 2, *tile), F32),
        pltpu.VMEM((SIDE, 2, *tile), F32),
        pltpu.VMEM((SIDE, 3, *tile), F32),
        pltpu.VMEM((SIDE, 3, *tile), F32),
        pltpu.VMEM((3, *tile), F32),
        pltpu.VMEM((SIDE, 3, *tile), F32),
        pltpu.VMEM((SIDE, 2, *tile), F32),
        pltpu.VMEM((SIDE, 2, *tile), F32),
        pltpu.VMEM(tile, F32),
        pltpu.VMEM((SIDE, *tile), F32),
        pltpu.VMEM(tile, F32),
        pltpu.VMEM((SIDE, *tile), F32),
        pltpu.VMEM((SIDE, SIDE, *part), BF16),
        pltpu.VMEM((SIDE, SIDE, *part), BF16),
        pltpu.VMEM((SIDE, SIDE, *part), BF16),
        pltpu.VMEM((SIDE, SIDE, *part), BF16),
        pltpu.VMEM((SIDE, *part), BF16),
        pltpu.VMEM((SIDE, *part), BF16),
        pltpu.VMEM((SIDE, *part), BF16),
        pltpu.VMEM((SIDE, *part), BF16),
        pltpu.VMEM((N_TP, D, DV), BF16),
        pltpu.VMEM((N_TP, TOK // N_TP, DV), BF16),
        pltpu.VMEM((N_TP, TOK // N_TP, DV), BF16),
        pltpu.SemaphoreType.DMA((KINDS,)),
        pltpu.SemaphoreType.DMA((KINDS,)),
        pltpu.SemaphoreType.DMA((7,)),
    ]
    shapes = (
        jax.ShapeDtypeStruct((DK, TOK), BF16),
        jax.ShapeDtypeStruct((DK, TOK), BF16),
        jax.ShapeDtypeStruct((2, 1, TOK), F32),
        jax.ShapeDtypeStruct((2, 1, TOK), F32),
        jax.ShapeDtypeStruct((ROWS, DV), F32),
        jax.ShapeDtypeStruct((TOK // N_TP, D), BF16),
    )
    results = pl.pallas_call(
        kernel,
        out_shape=shapes,
        in_specs=[outside] * 7,
        out_specs=[whole] * 6,
        scratch_shapes=scratch,
        compiler_params=pltpu.CompilerParams(
            collective_id=0, has_side_effects=True, vmem_limit_bytes=62 * 1024 * 1024
        ),
    )(features, value_weight, queries.T, key_vectors.T, log_input, log_forget, out_grad)
    written = pl.pallas_call(
        writer,
        out_shape=shapes,
        in_specs=[whole] * 6,
        out_specs=[outside] * 6,
        scratch_shapes=[pltpu.SemaphoreType.DMA((6,))],
        compiler_params=pltpu.CompilerParams(vmem_limit_bytes=4 * 1024 * 1024),
    )(*results)
    return (written[0].T, written[1].T, *written[2:])


def solution(mesh):
    placed = (
        P("sp", None),
        P(None, "tp"),
        P("sp", "tp"),
        P("sp", "tp"),
        P(None, "tp", "sp"),
        P(None, "tp", "sp"),
        P("sp", "tp"),
    )
    return jax.shard_map(
        body,
        mesh=mesh,
        in_specs=placed,
        out_specs=(
            P("sp", "tp"),
            P("sp", "tp"),
            P(None, "tp", "sp"),
            P(None, "tp", "sp"),
            P("sp", "tp"),
            P(("sp", "tp"), None),
        ),
        check_vma=False,
    )
```
